32 devices in a mesh: grp: 2 (over x), tp: 16 (over z, y, core).
Axes of the slice: x: 2, y: 2, z: 4, core: 2. Of those that a mesh axis runs over, the one named last changes fastest.
Arguments:
- tokens: bfloat16 [128, 4096], P('grp', 'tp'), parts along dimension 0, may hold values from -6 to 6
- lengths: int32 [128], P('grp'), parts along dimension 0, may hold values from 1 to 2048, as said below
- norm_gain: float32 [2, 4096], replicated, may hold values from 0.1 to 1.9
- in_weight: bfloat16 [2, 1024, 4096], P(None, 'tp'), may hold values from -0.09375 to 0.09375
- gate_weight: bfloat16 [2, 4096, 4096], P(None, 'tp'), may hold values from -0.09375 to 0.09375
- decay_rate: float32 [2, 64, 64], P(None, 'tp'), may hold values from 0.05 to 2
- frequency: float32 [2, 64, 64], P(None, 'tp'), may hold values from 0 to 201.06177
- log_step: float32 [2, 64], P(None, 'tp'), may hold values from -3 to 0
- input_map: float32 [2, 2, 64, 64, 16], P(None, None, 'tp'), may hold values from -1 to 1
- output_map: float32 [2, 2, 64, 16, 64], P(None, None, 'tp'), may hold values from -0.75 to 0.75
- skip_scale: float32 [2, 1024], P(None, 'tp'), may hold values from -4 to 4
- glu_weight: bfloat16 [2, 1024, 1024], P(None, 'tp'), may hold values from -0.1875 to 0.1875
- branch_weight: bfloat16 [2, 4096, 1024], P(None, 'tp'), may hold values from -0.1875 to 0.1875
- mix_weight: bfloat16 [2, 4096, 4096], P(None, 'tp'), may hold values from -0.09375 to 0.09375
- states: float32 [2, 2, 64, 64, 128], P(None, None, 'tp', None, 'grp'), parts along dimension 4, may hold values from -3 to 3
Outputs:
- mixed: bfloat16 [128, 4096], P('grp', 'tp'), parts along dimension 0
- new_states: float32 [2, 2, 64, 64, 128], P(None, None, 'tp', None, 'grp'), parts along dimension 4
The draws below stay inside these ranges and needn't reach their ends.
There are 2 independent parts, one for each index of `grp`. The reference program is written for one: setup_inputs(seed, part) draws one part's arguments, and reference() takes and returns one part's arrays. A program takes and returns all parts, laid end to end along the dimension named above; an argument that names none is the same for every part. Nothing has to cross between parts.
Inputs may be any that keep to these rules, and one draw needn't show every extreme that they name: `lengths`: one length is exactly 2048. Any number of sequences, from 1 to 64, may be longer than 512.
All inputs are finite; a program needn't handle non-finite values.
Results may differ from the reference program's by a relative error of at most 0.0085.
Values may be sent and summed in bfloat16 or wider, within the bound.
A program may use at most 64 MiB of HBM per device.

```python
import math
import jax
import jax.numpy as jnp
from jax import lax

D = 4096
G = 64
P_SIZE = 16
N = 64
LAYERS = 2
BATCH = 64
MEAN_LEN = 512
CH = 1024


def draw_lengths(key, part):
    spare = max(BATCH // 8, 1)
    full_count = BATCH - jax.random.randint(jax.random.fold_in(key, 11), (), 0, spare + 1)
    few_count = jax.random.randint(jax.random.fold_in(key, 12), (), 1, BATCH // 2 + 1)
    count = jnp.where(part % 2 == 0, full_count, few_count)
    order = jax.random.permutation(jax.random.fold_in(key, 13), BATCH)
    ranking = jnp.argsort(order, stable=True).astype(jnp.int32)
    long_len = jax.random.randint(jax.random.fold_in(key, 14), (BATCH,), MEAN_LEN + 1, 4 * MEAN_LEN + 1)
    short_len = jax.random.randint(jax.random.fold_in(key, 15), (BATCH,), 1, MEAN_LEN + 1)
    lengths = jnp.where(ranking < count, long_len, short_len)
    lengths = jnp.where(ranking == 0, 4 * MEAN_LEN, lengths)
    return lengths.astype(jnp.int32)


def level_of(stream_key, extent, split, least, high):
    factor_of = 1.0
    for axis_at, parts in split:
        draws = jax.random.uniform(jax.random.fold_in(jax.random.fold_in(stream_key, 6), axis_at), (parts,), jnp.float32, least / len(split), high / len(split))
        factor_of = factor_of * jnp.repeat(jnp.exp(draws), extent[axis_at] // parts).reshape((-1,) + (1,) * (len(extent) - 1 - axis_at))
    return factor_of


def noise(key, extent, scale, reach, cuts=(), kind=jnp.bfloat16):
    array = scale * jax.random.normal(key, extent, jnp.float32)
    if cuts:
        array = array * level_of(key, extent, cuts, -0.22, 0.18)
    return jnp.clip(array, -reach, reach).astype(kind)


def setup_inputs(seed: int = 0, part: int = 0) -> dict:
    streams_of = jax.random.split(jax.random.key(seed), 16)
    part_keys = jax.random.split(jax.random.fold_in(streams_of[15], part), 16)
    tokens = noise(part_keys[0], (BATCH, D), 1.0, 6.0, ((1, 16),))
    lengths = draw_lengths(jax.random.fold_in(jax.random.fold_in(streams_of[15], part), 71), part)
    norm_gain = jnp.clip(1.0 + 0.18 * jax.random.normal(streams_of[2], (LAYERS, D), jnp.float32), 0.1, 1.9)
    in_weight = noise(streams_of[3], (LAYERS, CH, D), D ** -0.5, 0.09375, ((1, 16),))
    gate_weight = noise(streams_of[4], (LAYERS, D, D), D ** -0.5, 0.09375, ((1, 16),))
    decay_rate = jnp.clip(jnp.exp(math.log(2.0) - 3.6888794 * jax.random.uniform(streams_of[5], (LAYERS, G, N), jnp.float32) ** level_of(streams_of[5], (LAYERS, G, N), ((1, 16),), -0.2, 0.2)), 0.05, 2.0)
    frequency = jnp.clip(201.06177 * jax.random.uniform(streams_of[6], (LAYERS, G, N), jnp.float32) ** level_of(streams_of[6], (LAYERS, G, N), ((1, 16),), -0.2, 0.2), 0.0, 201.06177)
    log_step = jnp.clip(-3.0 + 3.0 * jax.random.uniform(streams_of[7], (LAYERS, G), jnp.float32) ** level_of(streams_of[7], (LAYERS, G), ((1, 16),), -0.2, 0.2), -3.0, 0.0)
    input_map = noise(streams_of[8], (LAYERS, 2, G, N, P_SIZE), (2 * P_SIZE) ** -0.5, 1.0, ((2, 16),), jnp.float32)
    output_map = noise(streams_of[9], (LAYERS, 2, G, P_SIZE, N), N ** -0.5, 0.75, ((2, 16),), jnp.float32)
    skip_scale = noise(streams_of[10], (LAYERS, CH), 1.0, 4.0, ((1, 16),), jnp.float32)
    glu_weight = noise(streams_of[11], (LAYERS, CH, CH), CH ** -0.5, 0.1875, ((1, 16),))
    branch_weight = noise(streams_of[12], (LAYERS, D, CH), CH ** -0.5, 0.1875, ((1, 16),))
    mix_weight = noise(streams_of[13], (LAYERS, D, D), D ** -0.5, 0.09375, ((1, 16),))
    states = noise(part_keys[14], (LAYERS, 2, G, N, BATCH), 0.5, 3.0, ((2, 16),), jnp.float32)
    return dict(tokens=tokens, lengths=lengths, norm_gain=norm_gain, in_weight=in_weight, gate_weight=gate_weight, decay_rate=decay_rate, frequency=frequency, log_step=log_step, input_map=input_map, output_map=output_map, skip_scale=skip_scale, glu_weight=glu_weight, branch_weight=branch_weight, mix_weight=mix_weight, states=states)


EPS = 1e-06
HIGH = lax.Precision.HIGHEST

def discretize(decay_rate, frequency, log_step, input_map):
    step_len = jnp.exp(log_step)[:, None]
    real_part = -decay_rate
    magnitude = jnp.exp(real_part * step_len)
    decay_re = magnitude * jnp.cos(frequency * step_len)
    decay_im = magnitude * jnp.sin(frequency * step_len)
    denom = real_part * real_part + frequency * frequency
    factor_re = ((decay_re - 1.0) * real_part + decay_im * frequency) / denom
    factor_im = (decay_im * real_part - (decay_re - 1.0) * frequency) / denom
    drive_re = factor_re[..., None] * input_map[0] - factor_im[..., None] * input_map[1]
    drive_im = factor_re[..., None] * input_map[1] + factor_im[..., None] * input_map[0]
    return (decay_re, decay_im, drive_re, drive_im)

def recur(drive, live, decay_rate, frequency, log_step, input_map, output_map, skip_scale, carried):
    groups = decay_rate.shape[0]
    batch = drive.shape[0]
    decay_re, decay_im, drive_re, drive_im = discretize(decay_rate, frequency, log_step, input_map)
    grouped = drive.reshape(batch, groups, -1)
    push_re = jnp.einsum('gnp,bgp->gnb', drive_re, grouped, precision=HIGH)
    push_im = jnp.einsum('gnp,bgp->gnb', drive_im, grouped, precision=HIGH)
    new_re = decay_re[..., None] * carried[0] - decay_im[..., None] * carried[1] + push_re
    new_im = decay_re[..., None] * carried[1] + decay_im[..., None] * carried[0] + push_im
    new_re = jnp.where(live[None, None, :] > 0, new_re, carried[0])
    new_im = jnp.where(live[None, None, :] > 0, new_im, carried[1])
    read = jnp.einsum('gpn,gnb->bgp', output_map[0], new_re, precision=HIGH) - jnp.einsum('gpn,gnb->bgp', output_map[1], new_im, precision=HIGH) + skip_scale.reshape(groups, -1) * grouped
    activated = jax.nn.gelu(read.reshape(batch, -1)).astype(jnp.bfloat16)
    return (activated, jnp.stack([new_re, new_im]))

def reference(tokens, lengths, norm_gain, in_weight, gate_weight, decay_rate, frequency, log_step, input_map, output_map, skip_scale, glu_weight, branch_weight, mix_weight, states):
    live = (lengths > MEAN_LEN).astype(jnp.int32)
    current = tokens
    finals = []
    for layer in range(LAYERS):
        wide_in = current.astype(jnp.float32)
        inv_rms = lax.rsqrt(lax.optimization_barrier(jnp.sum(wide_in * wide_in, axis=1, keepdims=True)) / D + EPS)
        scaled = (wide_in * norm_gain[layer]).astype(jnp.bfloat16)
        drive = inv_rms * jnp.dot(scaled, in_weight[layer].T, preferred_element_type=jnp.float32)
        opening = jax.nn.sigmoid(inv_rms * jnp.dot(scaled, gate_weight[layer].T, preferred_element_type=jnp.float32))
        activated, fresh = recur(drive, live, decay_rate[layer], frequency[layer], log_step[layer], input_map[layer], output_map[layer], skip_scale[layer], states[layer])
        glu_pre = jnp.dot(activated, glu_weight[layer].T, preferred_element_type=jnp.float32)
        gated_units = (activated.astype(jnp.float32) * jax.nn.sigmoid(glu_pre)).astype(jnp.bfloat16)
        branch = jnp.dot(gated_units, branch_weight[layer].T, preferred_element_type=jnp.float32)
        weighted = (opening * branch).astype(jnp.bfloat16)
        update = jnp.dot(weighted, mix_weight[layer].T, preferred_element_type=jnp.float32)
        current = jnp.where(live[:, None] > 0, wide_in + update, wide_in).astype(jnp.bfloat16)
        finals.append(fresh)
    return (current, jnp.stack(finals))
```

```python
import functools

import jax
import jax.numpy as jnp
from jax import lax
from jax.experimental import pallas as pl
from jax.experimental.pallas import tpu as pltpu
from jax.sharding import PartitionSpec as P

MEAN_LEN = 512
EPS = 1e-06
HIGH = lax.Precision.HIGHEST
MESH = pl.DeviceIdType.MESH


def dot_nt(a, b, precision=None):
    return lax.dot_general(
        a, b, (((1,), (1,)), ((), ())), precision=precision, preferred_element_type=jnp.float32
    )


def dot_nn(a, b, precision=None):
    return lax.dot_general(
        a, b, (((1,), (0,)), ((), ())), precision=precision, preferred_element_type=jnp.float32
    )


def eye(n):
    return lax.broadcasted_iota(jnp.int32, (n, n), 0) == lax.broadcasted_iota(jnp.int32, (n, n), 1)


def to_col(row):
    n = row.shape[1]
    return jnp.sum(jnp.where(eye(n), jnp.broadcast_to(row, (n, n)), 0.0), axis=1, keepdims=True)


def to_row(col):
    n = col.shape[0]
    return jnp.sum(jnp.where(eye(n), jnp.broadcast_to(col, (n, n)), 0.0), axis=0, keepdims=True)


def kernel(
    dims,
    tokens,
    lengths,
    gain,
    skip,
    decay_rate,
    frequency,
    log_step,
    in_hbm,
    gate_hbm,
    input_hbm,
    output_hbm,
    glu_hbm,
    branch_hbm,
    mix_hbm,
    states_hbm,
    mixed,
    states_out,
    in_w,
    gate_w,
    glu_w,
    branch_w,
    mix_w,
    imap,
    omap,
    carried,
    xbuf,
    abuf,
    gbuf,
    wbuf,
    scaled,
    push_map,
    direct,
    base,
    load_sem,
    out_sem,
    send_sem,
    recv_sem,
):
    layers, zs, ys, cs = dims
    n = zs * ys * cs
    batch, width = tokens.shape
    features = width * n
    groups = decay_rate.shape[1]
    per = imap.shape[-1]
    chans = groups * per
    aligned = width % 128 == 0

    me = lax.axis_index("tp")
    core = lax.rem(me, cs)
    yy = lax.rem(me // cs, ys)
    zz = me // (cs * ys)

    def place(z, y, c):
        return (z * ys + y) * cs + c

    hops = sorted(range(1, zs), key=lambda d: (min(d, zs - d), d))
    across = [lax.rem(zz + d, zs) for d in hops]
    peers = [place(z, yy, core) for z in across]
    other_y = place(zz, 1 - yy, core) if ys > 1 else None
    partner = place(zz, yy, 1 - core) if cs > 1 else None
    greeted = peers + [p for p in (other_y, partner) if p is not None]

    barrier = pltpu.get_barrier_semaphore()
    for p in greeted:
        pl.semaphore_signal(barrier, inc=1, device_id={"tp": p}, device_id_type=MESH)

    def load(at, src, dst):
        copy = pltpu.make_async_copy(src, dst, load_sem.at[at])
        copy.start()
        return copy

    loads = {}
    count = 0
    plan = [("maps", None)]
    loads["imap"] = load(0, input_hbm, imap)
    loads["omap"] = load(1, output_hbm, omap)
    loads["states"] = load(2, states_hbm, carried)
    count = 3
    for layer in range(layers):
        for name, src, dst in (
            ("in", in_hbm, in_w),
            ("gate", gate_hbm, gate_w),
            ("glu", glu_hbm, glu_w),
            ("branch", branch_hbm, branch_w),
            ("mix", mix_hbm, mix_w),
        ):
            loads[name, layer] = load(count, src.at[layer], dst.at[layer])
            count += 1

    live_row = lengths[...] > MEAN_LEN
    live_row_f = jnp.where(live_row, 1.0, 0.0)
    live_col_f = to_col(live_row_f)
    live_col = live_col_f > 0.5

    sends = []

    def send(phase, buf, slot, target, slot_count):
        copy = pltpu.make_async_remote_copy(
            src_ref=buf.at[slot],
            dst_ref=buf.at[slot],
            send_sem=send_sem.at[phase, slot_count],
            recv_sem=recv_sem.at[phase, slot],
            device_id={"tp": target},
            device_id_type=MESH,
        )
        copy.start()
        sends.append(copy)

    def start(phase, buf):
        k = 0
        for p in list(reversed(peers)) + [p for p in (other_y, partner) if p is not None]:
            send(phase, buf, me, p, k)
            k += 1
        return k

    def arrive(phase, buf, slot):
        pltpu.make_async_remote_copy(
            src_ref=buf.at[slot],
            dst_ref=buf.at[slot],
            send_sem=send_sem.at[phase, 0],
            recv_sem=recv_sem.at[phase, slot],
            device_id={"tp": greeted[0]},
            device_id_type=MESH,
        ).wait_recv()

    def finish(phase, buf, k, each=None):
        def take(slot):
            if each is not None:
                each(slot)

        if each is not None:
            each(me)
        if ys > 1:
            arrive(phase, buf, other_y)
            if cs > 1:
                send(phase, buf, other_y, partner, k)
                k += 1
            take(other_y)
        for z in across:
            slot = place(z, yy, core)
            arrive(phase, buf, slot)
            if ys > 1:
                send(phase, buf, slot, other_y, k)
                k += 1
            if cs > 1:
                send(phase, buf, slot, partner, k)
                k += 1
            take(slot)
        if ys > 1:
            for z in across:
                slot = place(z, 1 - yy, core)
                arrive(phase, buf, slot)
                if cs > 1:
                    send(phase, buf, slot, partner, k)
                    k += 1
                take(slot)
        if cs > 1:
            order = [place(zz, yy, 1 - core)]
            if ys > 1:
                order.append(place(zz, 1 - yy, 1 - core))
            order += [place(z, yy, 1 - core) for z in across]
            if ys > 1:
                order += [place(z, 1 - yy, 1 - core) for z in across]
            for slot in order:
                arrive(phase, buf, slot)
                take(slot)

    def prepare(layer):
        step = log_step[layer : layer + 1, :]
        step_len = jnp.exp(to_col(step) if groups > 1 else step)
        real = -decay_rate[layer]
        freq = frequency[layer]
        magnitude = jnp.exp(real * step_len)
        decay_re = magnitude * jnp.cos(freq * step_len)
        decay_im = magnitude * jnp.sin(freq * step_len)
        denom = real * real + freq * freq
        factor_re = ((decay_re - 1.0) * real + decay_im * freq) / denom
        factor_im = (decay_im * real - (decay_re - 1.0) * freq) / denom
        res, ims, bases = [], [], []
        for g in range(groups):
            dre, dim, fre, fim = (
                to_col(v[g : g + 1, :]) for v in (decay_re, decay_im, factor_re, factor_im)
            )
            m0, m1 = imap[layer, 0, g], imap[layer, 1, g]
            res.append(fre * m0 - fim * m1)
            ims.append(fre * m1 + fim * m0)
            s0, s1 = carried[layer, 0, g], carried[layer, 1, g]
            kept_re = jnp.where(live_row, dre * s0 - dim * s1, s0)
            kept_im = jnp.where(live_row, dre * s1 + dim * s0, s1)
            carried[layer, 0, g] = kept_re
            carried[layer, 1, g] = kept_im
            bases.append(
                dot_nn(omap[layer, 0, g], kept_re, HIGH) - dot_nn(omap[layer, 1, g], kept_im, HIGH)
            )
        cat_re = jnp.concatenate(res, axis=1) if groups > 1 else res[0]
        cat_im = jnp.concatenate(ims, axis=1) if groups > 1 else ims[0]
        owner = lax.broadcasted_iota(jnp.int32, cat_re.shape, 1)
        for g in range(groups):
            mine = (owner >= g * per) & (owner < (g + 1) * per)
            map_re = jnp.where(mine, cat_re, 0.0)
            map_im = jnp.where(mine, cat_im, 0.0)
            push_map[layer, 0, g] = map_re
            push_map[layer, 1, g] = map_im
            direct[layer, pl.ds(g * per, per), :] = dot_nn(
                omap[layer, 0, g], map_re, HIGH
            ) - dot_nn(omap[layer, 1, g], map_im, HIGH)
        base_t = jnp.concatenate(bases, axis=0) if groups > 1 else bases[0]
        base[layer] = dot_nt(jnp.where(eye(batch), 1.0, 0.0), base_t, HIGH)

    def advance(layer, drive):
        for g in range(groups):
            for part in range(2):
                push = dot_nt(push_map[layer, part, g], drive, HIGH)
                kept = carried[layer, part, g]
                carried[layer, part, g] = jnp.where(live_row, kept + push, kept)
        out = pltpu.make_async_copy(carried.at[layer], states_out.at[layer], out_sem.at[layer])
        out.start()
        return out

    def cols(ref, layer, slot, size):
        if isinstance(slot, int):
            return ref[layer, :, slot * size : (slot + 1) * size]
        return ref[layer, :, pl.ds(pl.multiple_of(slot * size, size), size)]

    def wide(buf, layer):
        return jnp.concatenate([buf[layer, k] for k in range(n)], axis=1)

    xbuf[0, me] = tokens[...]
    pl.semaphore_wait(barrier, len(greeted))

    outs = []
    k = start(0, xbuf.at[0])
    loads["imap"].wait()
    loads["omap"].wait()
    loads["states"].wait()
    prepare(0)
    for layer in range(layers):
        phase = 4 * layer
        loads["in", layer].wait()
        sums = [jnp.zeros((batch, width), jnp.float32), jnp.zeros((batch, chans), jnp.float32)]

        def take_x(slot):
            x = xbuf[layer, slot].astype(jnp.float32)
            if isinstance(slot, int):
                g = gain[layer : layer + 1, slot * width : (slot + 1) * width]
            else:
                g = gain[layer : layer + 1, pl.ds(pl.multiple_of(slot * width, width), width)]
            piece = (x * g).astype(jnp.bfloat16)
            scaled[slot] = piece
            sums[0] = sums[0] + x * x
            sums[1] = sums[1] + dot_nt(piece, cols(in_w, layer, slot, width))

        finish(phase, xbuf.at[layer], k, take_x if aligned else None)
        if not aligned:
            for slot in range(n):
                take_x(slot)
        inv = lax.rsqrt(jnp.sum(sums[0], axis=1, keepdims=True) / features + EPS)
        drive = inv * sums[1]
        response = dot_nt(drive, direct[layer], HIGH)
        read = base[layer] + jnp.where(live_col, response, 0.0) + skip[layer : layer + 1, :] * drive
        activated = jax.nn.gelu(read).astype(jnp.bfloat16)
        abuf[layer, me] = activated
        k = start(phase + 1, abuf.at[layer])

        loads["gate", layer].wait()
        gate_acc = jnp.zeros((batch, width), jnp.float32)
        for slot in range(n):
            gate_acc = gate_acc + dot_nt(scaled[slot], cols(gate_w, layer, slot, width))
        opening = jax.nn.sigmoid(inv * gate_acc)

        loads["glu", layer].wait()
        finish(phase + 1, abuf.at[layer], k)
        glu_pre = dot_nt(wide(abuf, layer), glu_w[layer])
        gated = (activated.astype(jnp.float32) * jax.nn.sigmoid(glu_pre)).astype(jnp.bfloat16)
        gbuf[layer, me] = gated
        k = start(phase + 2, gbuf.at[layer])

        outs.append(advance(layer, drive))

        loads["branch", layer].wait()
        finish(phase + 2, gbuf.at[layer], k)
        branch = dot_nt(wide(gbuf, layer), branch_w[layer])
        wbuf[layer, me] = (opening * branch).astype(jnp.bfloat16)
        k = start(phase + 3, wbuf.at[layer])

        if layer + 1 < layers:
            prepare(layer + 1)
        loads["mix", layer].wait()
        total = [jnp.zeros((batch, width), jnp.float32)]

        def take_w(slot):
            total[0] = total[0] + dot_nt(wbuf[layer, slot], cols(mix_w, layer, slot, width))

        finish(phase + 3, wbuf.at[layer], k, take_w if aligned else None)
        if not aligned:
            for slot in range(n):
                take_w(slot)
        x_own = xbuf[layer, me].astype(jnp.float32)
        result = jnp.where(live_col, x_own + total[0], x_own).astype(jnp.bfloat16)
        if layer + 1 < layers:
            xbuf[layer + 1, me] = result
            k = start(phase + 4, xbuf.at[layer + 1])
        else:
            mixed[...] = result
    for copy in sends:
        copy.wait_send()
    for copy in outs:
        copy.wait()


def split_of(n):
    cs = 2 if n % 2 == 0 else 1
    ys = 2 if (n // cs) % 2 == 0 else 1
    return n // (cs * ys), ys, cs


def per_device(
    n,
    tokens,
    lengths,
    norm_gain,
    in_weight,
    gate_weight,
    decay_rate,
    frequency,
    log_step,
    input_map,
    output_map,
    skip_scale,
    glu_weight,
    branch_weight,
    mix_weight,
    states,
):
    batch, width = tokens.shape
    layers = in_weight.shape[0]
    groups, per = input_map.shape[2], input_map.shape[4]
    size = input_map.shape[3]
    chans = groups * per
    vmem = pl.BlockSpec(memory_space=pltpu.VMEM)
    hbm = pl.BlockSpec(memory_space=pl.ANY)
    bf16, f32 = jnp.bfloat16, jnp.float32
    return pl.pallas_call(
        functools.partial(kernel, (layers, *split_of(n))),
        out_shape=(
            jax.ShapeDtypeStruct(tokens.shape, bf16),
            jax.ShapeDtypeStruct(states.shape, f32),
        ),
        in_specs=[vmem] * 7 + [hbm] * 8,
        out_specs=(vmem, hbm),
        scratch_shapes=[
            pltpu.VMEM(in_weight.shape, bf16),
            pltpu.VMEM(gate_weight.shape, bf16),
            pltpu.VMEM(glu_weight.shape, bf16),
            pltpu.VMEM(branch_weight.shape, bf16),
            pltpu.VMEM(mix_weight.shape, bf16),
            pltpu.VMEM(input_map.shape, f32),
            pltpu.VMEM(output_map.shape, f32),
            pltpu.VMEM(states.shape, f32),
            pltpu.VMEM((layers, n, batch, width), bf16),
            pltpu.VMEM((layers, n, batch, chans), bf16),
            pltpu.VMEM((layers, n, batch, chans), bf16),
            pltpu.VMEM((layers, n, batch, width), bf16),
            pltpu.VMEM((n, batch, width), bf16),
            pltpu.VMEM((layers, 2, groups, size, chans), f32),
            pltpu.VMEM((layers, chans, chans), f32),
            pltpu.VMEM((layers, batch, chans), f32),
            pltpu.SemaphoreType.DMA((3 + 5 * layers,)),
            pltpu.SemaphoreType.DMA((layers,)),
            pltpu.SemaphoreType.DMA((4 * layers, n)),
            pltpu.SemaphoreType.DMA((4 * layers, n)),
        ],
        compiler_params=pltpu.CompilerParams(collective_id=0, has_side_effects=True),
        name="decode_layers",
    )(
        tokens,
        lengths.reshape(1, batch),
        norm_gain,
        skip_scale,
        decay_rate,
        frequency,
        log_step,
        in_weight,
        gate_weight,
        input_map,
        output_map,
        glu_weight,
        branch_weight,
        mix_weight,
        states,
    )


def solution(mesh):
    in_specs = (
        P("grp", "tp"),
        P("grp"),
        P(),
        P(None, "tp", None),
        P(None, "tp", None),
        P(None, "tp", None),
        P(None, "tp", None),
        P(None, "tp"),
        P(None, None, "tp", None, None),
        P(None, None, "tp", None, None),
        P(None, "tp"),
        P(None, "tp", None),
        P(None, "tp", None),
        P(None, "tp", None),
        P(None, None, "tp", None, "grp"),
    )
    out_specs = (P("grp", "tp"), P(None, None, "tp", None, "grp"))
    return jax.shard_map(
        functools.partial(per_device, mesh.shape["tp"]),
        mesh=mesh,
        in_specs=in_specs,
        out_specs=out_specs,
        check_vma=False,
    )
```

```python
import functools

import jax
import jax.numpy as jnp
from jax import lax
from jax.experimental import pallas as pl
from jax.experimental.pallas import tpu as pltpu
from jax.sharding import PartitionSpec as P

MEAN_LEN = 512
EPS = 1e-06
HIGH = lax.Precision.HIGHEST
MESH = pl.DeviceIdType.MESH
ROUTES = ("chip", "chip", "chip", "chip")


def dot_nt(a, b, precision=None):
    return lax.dot_general(
        a, b, (((1,), (1,)), ((), ())), precision=precision, preferred_element_type=jnp.float32
    )


def dot_nn(a, b, precision=None):
    return lax.dot_general(
        a, b, (((1,), (0,)), ((), ())), precision=precision, preferred_element_type=jnp.float32
    )


def eye(n):
    return lax.broadcasted_iota(jnp.int32, (n, n), 0) == lax.broadcasted_iota(jnp.int32, (n, n), 1)


def to_col(row):
    n = row.shape[1]
    return jnp.sum(jnp.where(eye(n), jnp.broadcast_to(row, (n, n)), 0.0), axis=1, keepdims=True)


def to_row(col):
    n = col.shape[0]
    return jnp.sum(jnp.where(eye(n), jnp.broadcast_to(col, (n, n)), 0.0), axis=0, keepdims=True)


def kernel(
    dims,
    tokens,
    lengths,
    gain,
    skip,
    decay_rate,
    frequency,
    log_step,
    in_hbm,
    gate_hbm,
    input_hbm,
    output_hbm,
    glu_hbm,
    branch_hbm,
    mix_hbm,
    states_hbm,
    mixed,
    states_out,
    in_w,
    gate_w,
    glu_w,
    branch_w,
    mix_w,
    imap,
    omap,
    carried,
    xbuf,
    abuf,
    gbuf,
    wbuf,
    scaled,
    push_map,
    direct,
    base,
    load_sem,
    out_sem,
    send_sem,
    recv_sem,
):
    layers, zs, ys, cs = dims
    n = zs * ys * cs
    batch, width = tokens.shape
    features = width * n
    groups = decay_rate.shape[1]
    per = imap.shape[-2]
    chans = groups * per
    aligned = width % 128 == 0

    me = lax.axis_index("tp")
    core = lax.rem(me, cs)
    yy = lax.rem(me // cs, ys)
    zz = me // (cs * ys)

    def place(z, y, c):
        return (z * ys + y) * cs + c

    hops = sorted(range(zs), key=lambda d: (min(d, zs - d), d))
    partner = [place(zz, yy, 1 - core)] if cs > 1 else []

    def away(dz, dy, dc):
        return place(lax.rem(zz + dz, zs), yy if dy == 0 else 1 - yy, core if dc == 0 else 1 - core)

    def route(kind):
        chips = [(dz, dy) for dz in hops for dy in range(ys) if (dz, dy) != (0, 0)]
        chips.sort(key=lambda h: min(h[0], zs - h[0]) + h[1])
        far = [away(dz, dy, 1) for dz, dy in chips] if cs > 1 else []
        if kind == "chip":
            near = [away(dz, dy, 0) for dz, dy in chips]
            return near[::-1] + partner, [(s, partner) for s in near] + [(s, []) for s in partner + far]
        twin = zz + 1 - 2 * lax.rem(zz, 2)
        across = [lax.rem(zz + d, zs) for d in range(2, zs, 2)]
        beyond = [lax.rem(twin + d, zs) for d in range(2, zs, 2)]
        side = away(0, 1, 0)

        def both(c):
            near = [place(twin, yy, c), place(twin, 1 - yy, c)]
            return near, [place(z, yy, c) for z in across], [place(z, yy, c) for z in beyond]

        near, column, outer = both(core)
        slant = [place(z, 1 - yy, core) for z in beyond]
        relayed = [place(z, 1 - yy, core) for z in across]
        legs = [(s, partner) for s in [side] + near]
        legs += [(s, [side] + partner) for s in column]
        legs += [(s, partner) for s in outer + slant + relayed]
        far = []
        if cs > 1:
            near2, column2, outer2 = both(1 - core)
            far = [away(0, 1, 1)] + near2 + column2 + outer2
            far += [place(z, 1 - yy, 1 - core) for z in beyond + across]
        first = column + slant + outer + near[::-1] + [side] + partner
        return first, legs + [(s, []) for s in partner + far]

    pairable = ys > 1 and zs % 2 == 0
    routes = [route(kind if kind != "mid" or pairable else "chip") for kind in ROUTES]
    greeted = [away(dz, dy, 0) for dz in hops for dy in range(ys) if (dz, dy) != (0, 0)] + partner

    barrier = pltpu.get_barrier_semaphore()
    for p in greeted:
        pl.semaphore_signal(barrier, inc=1, device_id={"tp": p}, device_id_type=MESH)

    def load(at, src, dst):
        copy = pltpu.make_async_copy(src, dst, load_sem.at[at])
        copy.start()
        return copy

    loads = {}
    count = 0
    loads["imap"] = load(0, input_hbm, imap)
    loads["omap"] = load(1, output_hbm, omap)
    loads["states"] = load(2, states_hbm, carried)
    count = 3
    for layer in range(layers):
        for name, src, dst in (
            ("in", in_hbm, in_w),
            ("gate", gate_hbm, gate_w),
            ("glu", glu_hbm, glu_w),
            ("branch", branch_hbm, branch_w),
            ("mix", mix_hbm, mix_w),
        ):
            loads[name, layer] = load(count, src.at[layer], dst.at[layer])
            count += 1

    live_row = lengths[...] > MEAN_LEN
    live_row_f = jnp.where(live_row, 1.0, 0.0)
    live_col_f = to_col(live_row_f)
    live_col = live_col_f > 0.5

    sends = []

    def send(phase, buf, slot, target, slot_count):
        copy = pltpu.make_async_remote_copy(
            src_ref=buf.at[slot],
            dst_ref=buf.at[slot],
            send_sem=send_sem.at[phase, slot_count],
            recv_sem=recv_sem.at[phase, slot],
            device_id={"tp": target},
            device_id_type=MESH,
        )
        copy.start()
        sends.append(copy)

    def start(phase, buf):
        targets = routes[phase % 4][0]
        for k, p in enumerate(targets):
            send(phase, buf, me, p, k)
        return len(targets)

    def arrive(phase, buf, slot):
        pltpu.make_async_remote_copy(
            src_ref=buf.at[slot],
            dst_ref=buf.at[slot],
            send_sem=send_sem.at[phase, 0],
            recv_sem=recv_sem.at[phase, slot],
            device_id={"tp": greeted[0]},
            device_id_type=MESH,
        ).wait_recv()

    def finish(phase, buf, k, each=None):
        if each is not None:
            each(me)
        for slot, targets in routes[phase % 4][1]:
            arrive(phase, buf, slot)
            for p in targets:
                send(phase, buf, slot, p, k)
                k += 1
            if each is not None:
                each(slot)

    def prepare(layer):
        step = log_step[layer : layer + 1, :]
        step_len = jnp.exp(to_col(step) if groups > 1 else step)
        real = -decay_rate[layer]
        freq = frequency[layer]
        magnitude = jnp.exp(real * step_len)
        decay_re = magnitude * jnp.cos(freq * step_len)
        decay_im = magnitude * jnp.sin(freq * step_len)
        denom = real * real + freq * freq
        factor_re = ((decay_re - 1.0) * real + decay_im * freq) / denom
        factor_im = (decay_im * real - (decay_re - 1.0) * freq) / denom
        res, ims, bases = [], [], []
        for g in range(groups):
            dre, dim = to_col(decay_re[g : g + 1, :]), to_col(decay_im[g : g + 1, :])
            fre, fim = factor_re[g : g + 1, :], factor_im[g : g + 1, :]
            m0, m1 = imap[layer, 0, g], imap[layer, 1, g]
            res.append(fre * m0 - fim * m1)
            ims.append(fre * m1 + fim * m0)
            s0, s1 = carried[layer, 0, g], carried[layer, 1, g]
            kept_re = jnp.where(live_row, dre * s0 - dim * s1, s0)
            kept_im = jnp.where(live_row, dre * s1 + dim * s0, s1)
            carried[layer, 0, g] = kept_re
            carried[layer, 1, g] = kept_im
            bases.append(
                dot_nn(omap[layer, 0, g], kept_re, HIGH) - dot_nn(omap[layer, 1, g], kept_im, HIGH)
            )
        cat_re = jnp.concatenate(res, axis=0) if groups > 1 else res[0]
        cat_im = jnp.concatenate(ims, axis=0) if groups > 1 else ims[0]
        unit = jnp.where(eye(cat_re.shape[1]), 1.0, 0.0)
        turned_re, turned_im = dot_nt(unit, cat_re, HIGH), dot_nt(unit, cat_im, HIGH)
        owner = lax.broadcasted_iota(jnp.int32, turned_re.shape, 1)
        source = lax.broadcasted_iota(jnp.int32, (per, chans), 1)
        for g in range(groups):
            mine = (owner >= g * per) & (owner < (g + 1) * per)
            push_map[layer, 0, g] = jnp.where(mine, turned_re, 0.0)
            push_map[layer, 1, g] = jnp.where(mine, turned_im, 0.0)
            block = dot_nt(omap[layer, 0, g], cat_re, HIGH) - dot_nt(omap[layer, 1, g], cat_im, HIGH)
            here = (source >= g * per) & (source < (g + 1) * per)
            direct[layer, pl.ds(g * per, per), :] = jnp.where(here, block, 0.0)
        base_t = jnp.concatenate(bases, axis=0) if groups > 1 else bases[0]
        base[layer] = dot_nt(jnp.where(eye(batch), 1.0, 0.0), base_t, HIGH)

    def advance(layer, drive):
        for g in range(groups):
            for part in range(2):
                push = dot_nt(push_map[layer, part, g], drive, HIGH)
                kept = carried[layer, part, g]
                carried[layer, part, g] = jnp.where(live_row, kept + push, kept)
        out = pltpu.make_async_copy(carried.at[layer], states_out.at[layer], out_sem.at[layer])
        out.start()
        return out

    def cols(ref, layer, slot, size):
        if isinstance(slot, int):
            return ref[layer, :, slot * size : (slot + 1) * size]
        return ref[layer, :, pl.ds(pl.multiple_of(slot * size, size), size)]

    half = batch // 2

    def pack(block):
        return jnp.concatenate([block[:half], block[half:]], axis=1)

    def wide(buf, layer):
        blocks = [buf[layer, k] for k in range(n)]
        top = jnp.concatenate([block[:, :chans] for block in blocks], axis=1)
        low = jnp.concatenate([block[:, chans:] for block in blocks], axis=1)
        return jnp.concatenate([top, low], axis=0)

    xbuf[0, me] = tokens[...]
    pl.semaphore_wait(barrier, len(greeted))

    outs = []
    k = start(0, xbuf.at[0])
    loads["imap"].wait()
    loads["omap"].wait()
    loads["states"].wait()
    prepare(0)
    for layer in range(layers):
        phase = 4 * layer
        loads["in", layer].wait()
        sums = [jnp.zeros((batch, width), jnp.float32), jnp.zeros((batch, chans), jnp.float32)]

        def take_x(slot):
            x = xbuf[layer, slot].astype(jnp.float32)
            if isinstance(slot, int):
                g = gain[layer : layer + 1, slot * width : (slot + 1) * width]
            else:
                g = gain[layer : layer + 1, pl.ds(pl.multiple_of(slot * width, width), width)]
            piece = (x * g).astype(jnp.bfloat16)
            scaled[slot] = piece
            sums[0] = sums[0] + x * x
            sums[1] = sums[1] + dot_nt(piece, cols(in_w, layer, slot, width))

        finish(phase, xbuf.at[layer], k, take_x if aligned else None)
        if not aligned:
            for slot in range(n):
                take_x(slot)
        inv = lax.rsqrt(jnp.sum(sums[0], axis=1, keepdims=True) / features + EPS)
        drive = inv * sums[1]
        response = dot_nt(drive, direct[layer], HIGH)
        read = base[layer] + jnp.where(live_col, response, 0.0) + skip[layer : layer + 1, :] * drive
        activated = jax.nn.gelu(read).astype(jnp.bfloat16)
        abuf[layer, me] = pack(activated)
        k = start(phase + 1, abuf.at[layer])

        loads["gate", layer].wait()
        gate_acc = jnp.zeros((batch, width), jnp.float32)
        for slot in range(n):
            gate_acc = gate_acc + dot_nt(scaled[slot], cols(gate_w, layer, slot, width))
        opening = jax.nn.sigmoid(inv * gate_acc)

        loads["glu", layer].wait()
        finish(phase + 1, abuf.at[layer], k)
        glu_pre = dot_nt(wide(abuf, layer), glu_w[layer])
        gated = (activated.astype(jnp.float32) * jax.nn.sigmoid(glu_pre)).astype(jnp.bfloat16)
        gbuf[layer, me] = pack(gated)
        k = start(phase + 2, gbuf.at[layer])

        outs.append(advance(layer, drive))

        loads["branch", layer].wait()
        finish(phase + 2, gbuf.at[layer], k)
        branch = dot_nt(wide(gbuf, layer), branch_w[layer])
        wbuf[layer, me] = (opening * branch).astype(jnp.bfloat16)
        k = start(phase + 3, wbuf.at[layer])

        if layer + 1 < layers:
            prepare(layer + 1)
        loads["mix", layer].wait()
        total = [jnp.zeros((batch, width), jnp.float32)]

        def take_w(slot):
            total[0] = total[0] + dot_nt(wbuf[layer, slot], cols(mix_w, layer, slot, width))

        finish(phase + 3, wbuf.at[layer], k, take_w if aligned else None)
        if not aligned:
            for slot in range(n):
                take_w(slot)
        x_own = xbuf[layer, me].astype(jnp.float32)
        result = jnp.where(live_col, x_own + total[0], x_own).astype(jnp.bfloat16)
        if layer + 1 < layers:
            xbuf[layer + 1, me] = result
            k = start(phase + 4, xbuf.at[layer + 1])
        else:
            mixed[...] = result
    for copy in sends:
        copy.wait_send()
    for copy in outs:
        copy.wait()


def hand_over(mixed, states, mixed_out, states_out):
    mixed_out[...] = mixed[...]
    states_out[...] = states[...]


def split_of(n):
    cs = 2 if n % 2 == 0 else 1
    ys = 2 if (n // cs) % 2 == 0 else 1
    return n // (cs * ys), ys, cs


def per_device(
    n,
    tokens,
    lengths,
    norm_gain,
    in_weight,
    gate_weight,
    decay_rate,
    frequency,
    log_step,
    input_map,
    output_map,
    skip_scale,
    glu_weight,
    branch_weight,
    mix_weight,
    states,
):
    batch, width = tokens.shape
    layers = in_weight.shape[0]
    groups, per = input_map.shape[2], input_map.shape[4]
    size = input_map.shape[3]
    chans = groups * per
    vmem = pl.BlockSpec(memory_space=pltpu.VMEM)
    hbm = pl.BlockSpec(memory_space=pl.ANY)
    bf16, f32 = jnp.bfloat16, jnp.float32
    mixed, finals = pl.pallas_call(
        functools.partial(kernel, (layers, *split_of(n))),
        out_shape=(
            jax.ShapeDtypeStruct(tokens.shape, bf16),
            jax.ShapeDtypeStruct(states.shape, f32),
        ),
        in_specs=[vmem] * 7 + [hbm] * 8,
        out_specs=(vmem, hbm),
        scratch_shapes=[
            pltpu.VMEM(in_weight.shape, bf16),
            pltpu.VMEM(gate_weight.shape, bf16),
            pltpu.VMEM(glu_weight.shape, bf16),
            pltpu.VMEM(branch_weight.shape, bf16),
            pltpu.VMEM(mix_weight.shape, bf16),
            pltpu.VMEM((layers, 2, groups, per, size), f32),
            pltpu.VMEM(output_map.shape, f32),
            pltpu.VMEM(states.shape, f32),
            pltpu.VMEM((layers, n, batch, width), bf16),
            pltpu.VMEM((layers, n, batch // 2, 2 * chans), bf16),
            pltpu.VMEM((layers, n, batch // 2, 2 * chans), bf16),
            pltpu.VMEM((layers, n, batch, width), bf16),
            pltpu.VMEM((n, batch, width), bf16),
            pltpu.VMEM((layers, 2, groups, size, chans), f32),
            pltpu.VMEM((layers, chans, chans), f32),
            pltpu.VMEM((layers, batch, chans), f32),
            pltpu.SemaphoreType.DMA((3 + 5 * layers,)),
            pltpu.SemaphoreType.DMA((layers,)),
            pltpu.SemaphoreType.DMA((4 * layers, n)),
            pltpu.SemaphoreType.DMA((4 * layers, n)),
        ],
        compiler_params=pltpu.CompilerParams(collective_id=0, has_side_effects=True),
        name="decode_layers",
    )(
        tokens,
        lengths.reshape(1, batch),
        norm_gain,
        skip_scale,
        decay_rate,
        frequency,
        log_step,
        in_weight,
        gate_weight,
        jnp.swapaxes(input_map, 3, 4),
        output_map,
        glu_weight,
        branch_weight,
        mix_weight,
        states,
    )
    return pl.pallas_call(
        hand_over,
        out_shape=(
            jax.ShapeDtypeStruct(tokens.shape, bf16),
            jax.ShapeDtypeStruct(states.shape, f32),
        ),
        in_specs=[vmem] * 2,
        out_specs=(vmem,) * 2,
        name="hand_over",
    )(mixed, finals)


def solution(mesh):
    in_specs = (
        P("grp", "tp"),
        P("grp"),
        P(),
        P(None, "tp", None),
        P(None, "tp", None),
        P(None, "tp", None),
        P(None, "tp", None),
        P(None, "tp"),
        P(None, None, "tp", None, None),
        P(None, None, "tp", None, None),
        P(None, "tp"),
        P(None, "tp", None),
        P(None, "tp", None),
        P(None, "tp", None),
        P(None, None, "tp", None, "grp"),
    )
    out_specs = (P("grp", "tp"), P(None, None, "tp", None, "grp"))
    return jax.shard_map(
        functools.partial(per_device, mesh.shape["tp"]),
        mesh=mesh,
        in_specs=in_specs,
        out_specs=out_specs,
        check_vma=False,
    )
```
